32 devices in a mesh: kv: 8 (over z, y), tp: 4 (over x, core).
Axes of the slice: x: 2, y: 2, z: 4, core: 2. Of those that a mesh axis runs over, the one named last changes fastest.
Arguments:
- tokens: bfloat16 [64, 4096], P(None, 'kv'), may hold values from -8 to 8
- attn_gain: float32 [4096], P('kv'), may hold values from 0.1 to 1.9
- w_query: bfloat16 [4096, 2048], P('kv', 'tp'), may hold values from -0.09375 to 0.09375
- w_key: bfloat16 [4096, 2048], P('kv', 'tp'), may hold values from -0.09375 to 0.09375
- w_value: bfloat16 [4096, 4096], P('kv', 'tp'), may hold values from -0.09375 to 0.09375
- w_outgate: bfloat16 [4096, 4096], P('kv', 'tp'), may hold values from -0.09375 to 0.09375
- w_gates: bfloat16 [4096, 16], replicated, may hold values from -0.029907227 to 0.029907227
- forget_bias: float32 [8], replicated, may hold values from -1 to 3
- state_c: float32 [64, 8, 512, 256], P('kv', 'tp'), may hold values from -6 to 6
- state_n: float32 [64, 8, 256], P('kv', 'tp'), may hold values from -6 to 6
- state_m: float32 [64, 8], P('kv', 'tp'), may hold values from -2 to 0.5
- w_output: bfloat16 [4096, 4096], P('tp', 'kv'), may hold values from -0.09375 to 0.09375
- mlp_gain: float32 [4096], P('kv'), may hold values from 0.1 to 1.9
- w_gateff: bfloat16 [4096, 11008], P('kv', 'tp'), may hold values from -0.09375 to 0.09375
- w_upff: bfloat16 [4096, 11008], P('kv', 'tp'), may hold values from -0.09375 to 0.09375
- w_downff: bfloat16 [11008, 4096], P('tp', 'kv'), may hold values from -0.0546875 to 0.0546875
Outputs:
- mixed: bfloat16 [64, 4096], P(None, 'kv')
- new_c: float32 [64, 8, 512, 256], P('kv', 'tp')
- new_n: float32 [64, 8, 256], P('kv', 'tp')
- new_m: float32 [64, 8], P('kv', 'tp')
The draws below stay inside these ranges and needn't reach their ends.
All inputs are finite; a program needn't handle non-finite values.
Results may differ from the reference program's by a relative error of at most 0.0083.
Values may be sent and summed in bfloat16 or wider, within the bound.
A program may use at most 64 MiB of HBM per device.

```python
import math
import jax
import jax.numpy as jnp
from jax import lax

D = 4096
HEADS = 8
DQK = 256
DV = 512
FF = 11008
BATCH = 64


def draw_tokens(key, part):
    key_scale = jax.random.fold_in(key, 11)
    key_values = jax.random.fold_in(key, 12)
    groups = D // 16
    scales = jnp.exp(jax.random.uniform(key_scale, (groups,), jnp.float32, math.log(0.3), math.log(3.0)))
    scales = jnp.repeat(scales, 16)
    values = jax.random.normal(key_values, (BATCH, D), jnp.float32)
    return jnp.clip(values * scales[None, :], -8.0, 8.0).astype(jnp.bfloat16)


def level_of(rng, extent, shards, smallest, largest):
    def one(position, blocks):
        heights = jax.random.uniform(jax.random.fold_in(jax.random.fold_in(rng, 6), position), (blocks,), jnp.float32, smallest / len(shards), largest / len(shards))
        return jnp.repeat(jnp.exp(heights), extent[position] // blocks).reshape((-1,) + (1,) * (len(extent) - position - 1))

    loudness = one(*shards[0])
    for cut in shards[1:]:
        loudness = loudness * one(*cut)
    return loudness


def normal_values(stream_key, extent, deviation, limit, pieces=(), held_as=jnp.bfloat16):
    entries = jax.random.normal(stream_key, extent, jnp.float32) * deviation
    if len(pieces) > 0:
        entries = level_of(stream_key, extent, pieces, -0.22, 0.18) * entries
    return jnp.clip(entries, min=-limit, max=limit).astype(held_as)


def setup_inputs(seed: int = 0) -> dict:
    streams_of = jax.random.split(jax.random.key(seed), 17)
    return {
        "tokens": draw_tokens(jax.random.fold_in(streams_of[16], 71), 0),
        "attn_gain": jnp.clip(1.0 + 0.18 * jax.random.normal(streams_of[1], (D,), jnp.float32), 0.1, 1.9),
        "w_query": normal_values(streams_of[2], (D, HEADS * DQK), D ** -0.5, 0.09375, ((0, 8), (1, 4))),
        "w_key": normal_values(streams_of[3], (D, HEADS * DQK), D ** -0.5, 0.09375, ((0, 8), (1, 4))),
        "w_value": normal_values(streams_of[4], (D, HEADS * DV), D ** -0.5, 0.09375, ((0, 8), (1, 4))),
        "w_outgate": normal_values(streams_of[5], (D, HEADS * DV), D ** -0.5, 0.09375, ((0, 8), (1, 4))),
        "w_gates": normal_values(streams_of[6], (D, 2 * HEADS), 0.0047, 0.029907227),
        "forget_bias": jnp.clip(jax.random.uniform(streams_of[7], (HEADS,), jnp.float32, -1.0, 3.0), -1.0, 3.0),
        "state_c": normal_values(streams_of[8], (BATCH, HEADS, DV, DQK), 1.0, 6.0, ((0, 8), (1, 4)), jnp.float32),
        "state_n": normal_values(streams_of[9], (BATCH, HEADS, DQK), 1.0, 6.0, ((0, 8), (1, 4)), jnp.float32),
        "state_m": jnp.clip(-2.0 + 2.5 * jax.random.uniform(streams_of[10], (BATCH, HEADS), jnp.float32) ** level_of(streams_of[10], (BATCH, HEADS), ((0, 8), (1, 4)), -0.2, 0.2), -2.0, 0.5),
        "w_output": normal_values(streams_of[11], (HEADS * DV, D), (HEADS * DV) ** -0.5, 0.09375, ((0, 4), (1, 8))),
        "mlp_gain": jnp.clip(1.0 + 0.18 * jax.random.normal(streams_of[12], (D,), jnp.float32), 0.1, 1.9),
        "w_gateff": normal_values(streams_of[13], (D, FF), D ** -0.5, 0.09375, ((0, 8), (1, 4))),
        "w_upff": normal_values(streams_of[14], (D, FF), D ** -0.5, 0.09375, ((0, 8), (1, 4))),
        "w_downff": normal_values(streams_of[15], (FF, D), FF ** -0.5, 0.0546875, ((0, 4), (1, 8))),
    }


norm_floor = 1e-05

def inverse_rms(values):
    return lax.rsqrt(lax.optimization_barrier(jnp.mean(values * values, axis=-1)) + norm_floor)

def reference(tokens, attn_gain, w_query, w_key, w_value, w_outgate, w_gates, forget_bias, state_c, state_n, state_m, w_output, mlp_gain, w_gateff, w_upff, w_downff):
    batch = tokens.shape[0]
    tok_float = tokens.astype(jnp.float32)
    scale_one = inverse_rms(tok_float)[:, None]
    normed_one = (tok_float * attn_gain).astype(jnp.bfloat16)

    def project(weight):
        return jnp.dot(normed_one, weight, preferred_element_type=jnp.float32) * scale_one
    query = (project(w_query) * DQK ** (-0.5)).reshape(batch, HEADS, DQK)
    key_vec = project(w_key).reshape(batch, HEADS, DQK)
    value = project(w_value).reshape(batch, HEADS, DV)
    out_pre = project(w_outgate).reshape(batch, HEADS, DV)
    gate_pre = project(w_gates)
    log_input = gate_pre[:, :HEADS]
    log_forget = jax.nn.log_sigmoid(gate_pre[:, HEADS:] + forget_bias)
    carried = log_forget + state_m
    new_m = jnp.maximum(carried, log_input)
    keep = jnp.exp(carried - new_m)
    admit = jnp.exp(log_input - new_m)
    new_c = keep[:, :, None, None] * state_c + admit[:, :, None, None] * value[:, :, :, None] * key_vec[:, :, None, :]
    new_n = keep[:, :, None] * state_n + admit[:, :, None] * key_vec
    numer = jnp.einsum('bhvd,bhd->bhv', new_c, query, precision=lax.Precision.HIGHEST)
    denom = jnp.maximum(jnp.abs(lax.optimization_barrier(jnp.sum(new_n * query, axis=-1))), jnp.exp(-new_m))
    head_out = (jax.nn.sigmoid(out_pre) * numer / denom[:, :, None]).reshape(batch, HEADS * DV).astype(jnp.bfloat16)
    attn_mix = jnp.dot(head_out, w_output, preferred_element_type=jnp.float32)
    middle = (tok_float + attn_mix).astype(jnp.bfloat16)
    mid_float = middle.astype(jnp.float32)
    scale_two = inverse_rms(mid_float)[:, None]
    normed_two = (mid_float * mlp_gain).astype(jnp.bfloat16)
    gate_ff = jnp.dot(normed_two, w_gateff, preferred_element_type=jnp.float32) * scale_two
    up_ff = jnp.dot(normed_two, w_upff, preferred_element_type=jnp.float32) * scale_two
    hidden_ff = (jax.nn.silu(gate_ff) * up_ff).astype(jnp.bfloat16)
    mixed = (mid_float + jnp.dot(hidden_ff, w_downff, preferred_element_type=jnp.float32)).astype(jnp.bfloat16)
    return (mixed, new_c, new_n, new_m)
```

```python
import jax
import jax.numpy as jnp
from jax import lax
from jax.experimental import pallas as pl
from jax.experimental.pallas import tpu as pltpu
from jax.sharding import PartitionSpec as P

norm_floor = 1e-05
MESH = pl.DeviceIdType.MESH
LANES = 128
CHUNK = 512
VMEM_SPEC = pl.BlockSpec(memory_space=pltpu.VMEM)
HBM_SPEC = pl.BlockSpec(memory_space=pltpu.HBM)


def pieces(total):
    return [(at, min(CHUNK, total - at)) for at in range(0, total, CHUNK)]


def peer_of(axis, step):
    count = lax.axis_size(axis)
    return lax.rem(lax.axis_index(axis) + step, count)


def signal_peers(barrier, axis):
    for step in range(1, lax.axis_size(axis)):
        pl.semaphore_signal(
            barrier, inc=1, device_id={axis: peer_of(axis, step)}, device_id_type=MESH
        )


def remote(axis, step, src, dst, send_sem, recv_sem):
    return pltpu.make_async_remote_copy(
        src_ref=src,
        dst_ref=dst,
        send_sem=send_sem,
        recv_sem=recv_sem,
        device_id={axis: peer_of(axis, step)},
        device_id_type=MESH,
    )


def project_kernel(
    tok_ref, gain_ref, wq, wk, wv, wo, wg,
    proj_ref, gate_ref,
    wq_v, wk_v, wv_v, wo_v, wg_v, part, land, gpart, gland,
    load_sem, send_sem, recv_sem, gsend_sem, grecv_sem,
):
    kv = lax.axis_index("kv")
    count = lax.axis_size("kv")
    batch, width = tok_ref.shape
    rows = batch // count
    weights = [(wq, wq_v), (wk, wk_v), (wv, wv_v), (wo, wo_v)]
    loads = [
        pltpu.make_async_copy(wg.at[:, pl.ds(pl.multiple_of(kv * width, LANES), width)], wg_v, load_sem.at[len(weights)])
    ]
    loads += [
        pltpu.make_async_copy(src, dst, load_sem.at[i]) for i, (src, dst) in enumerate(weights)
    ]
    for load in loads:
        load.start()
    barrier = pltpu.get_barrier_semaphore()
    signal_peers(barrier, "kv")
    tok = tok_ref[...].astype(jnp.float32)
    squares = jnp.sum(tok * tok, axis=1, keepdims=True)
    normed = (tok * gain_ref[...]).astype(jnp.bfloat16)
    loads[0].wait()
    gates = lax.dot_general(
        normed, wg_v[...], (((1,), (1,)), ((), ())), preferred_element_type=jnp.float32
    )
    gate_cols = gates.shape[1]
    gpart[...] = jnp.broadcast_to(squares, (batch, LANES)).reshape(count, rows, LANES)
    gpart[:, :, :gate_cols] = gates.reshape(count, rows, gate_cols)
    pl.semaphore_wait(barrier, count - 1)
    copies = []
    for step in range(1, count):
        copy = remote(
            "kv", step, gpart.at[peer_of("kv", step)], gland.at[step],
            gsend_sem.at[step], grecv_sem.at[step],
        )
        copy.start()
        copies.append(copy)
    at = 0
    spans = []
    for i, (_, dst) in enumerate(weights):
        loads[i + 1].wait()
        wide = dst.shape[1]
        for off, size in pieces(wide):
            out = jnp.dot(normed, dst[:, off : off + size], preferred_element_type=jnp.float32)
            part[:, :, at + off : at + off + size] = out.reshape(count, rows, size).astype(
                jnp.bfloat16
            )
        span = pl.ds(at, wide)
        group = []
        for step in range(1, count):
            copy = remote(
                "kv", step, part.at[peer_of("kv", step), :, span], land.at[step, :, span],
                send_sem.at[i, step], recv_sem.at[i, step],
            )
            copy.start()
            group.append(copy)
        spans.append((at, wide, group))
        at += wide
    total = gpart[kv]
    for copy in copies:
        copy.wait_recv()
    for step in range(1, count):
        total += gland[step]
    mean = total[:, gate_cols : gate_cols + 1] / (width * count)
    scale = lax.rsqrt(mean + norm_floor)
    gate_ref[...] = total * scale
    for at, wide, group in spans:
        for copy in group:
            copy.wait_recv()
        acc = part[kv, :, at : at + wide].astype(jnp.float32)
        for step in range(1, count):
            acc += land[step, :, at : at + wide].astype(jnp.float32)
        proj_ref[:, at : at + wide] = acc * scale
    for copy in copies:
        copy.wait_send()
    for _, _, group in spans:
        for copy in group:
            copy.wait_send()


def state_kernel(
    proj_ref, gate_ref, bias_ref, m_ref, n_ref, c_hbm,
    head_ref, newn_ref, newm_ref, newc_hbm,
    held, in_sem, out_sem,
):
    rows, heads, value_size, query_size = held.shape
    tp = lax.axis_index("tp")
    heads_all = bias_ref.shape[1]
    slots = [(h, b) for h in range(heads) for b in range(rows)]
    loads = [
        pltpu.make_async_copy(c_hbm.at[b, h], held.at[b, h], in_sem.at[b, h]) for h, b in slots
    ]
    for load in loads:
        load.start()
    gates = gate_ref[...]
    lane = lax.broadcasted_iota(jnp.int32, gates.shape, 1)
    bias_lane = lax.broadcasted_iota(jnp.int32, bias_ref.shape, 1)
    sub = lax.broadcasted_iota(jnp.int32, (rows, value_size), 0)
    query_width = heads * query_size
    value_at = 2 * query_width
    out_at = value_at + heads * value_size
    stores = []
    for h in range(heads):
        column = tp * heads + h
        log_input = jnp.sum(jnp.where(lane == column, gates, 0.0), axis=1, keepdims=True)
        forget = jnp.sum(jnp.where(lane == heads_all + column, gates, 0.0), axis=1, keepdims=True)
        bias = jnp.sum(jnp.where(bias_lane == column, bias_ref[...], 0.0), axis=1, keepdims=True)
        pre = forget + bias
        log_forget = jnp.minimum(pre, 0.0) - jnp.log(1.0 + jnp.exp(-jnp.abs(pre)))
        carried = log_forget + m_ref[:, h : h + 1]
        new_m = jnp.maximum(carried, log_input)
        keep = jnp.exp(carried - new_m)
        admit = jnp.exp(log_input - new_m)
        newm_ref[:, h : h + 1] = new_m
        query = proj_ref[:, h * query_size : (h + 1) * query_size] * query_size ** (-0.5)
        key_at = query_width + h * query_size
        key = admit * proj_ref[:, key_at : key_at + query_size]
        v_at = value_at + h * value_size
        value = proj_ref[:, v_at : v_at + value_size]
        o_at = out_at + h * value_size
        out_pre = proj_ref[:, o_at : o_at + value_size]
        new_n = keep * n_ref[:, h, :] + key
        newn_ref[:, h, :] = new_n
        value_cols = value.T
        keep_wide = jnp.broadcast_to(keep, (rows, query_size))
        query_low = query.astype(jnp.bfloat16)
        read = jnp.zeros((rows, value_size), jnp.float32)
        for b in range(rows):
            i = h * rows + b
            loads[i].wait()
            old = held[b, h]
            one = lax.dot_general(
                query_low, old.astype(jnp.bfloat16), (((1,), (1,)), ((), ())),
                preferred_element_type=jnp.float32,
            )
            read = jnp.where(sub == b, one, read)
            held[b, h] = (
                keep_wide[b : b + 1, :] * old + value_cols[:, b : b + 1] * key[b : b + 1, :]
            )
            store = pltpu.make_async_copy(held.at[b, h], newc_hbm.at[b, h], out_sem.at[b, h])
            store.start()
            stores.append(store)
        numer = keep * read + value * jnp.sum(key * query, axis=1, keepdims=True)
        denom = jnp.maximum(
            jnp.abs(jnp.sum(new_n * query, axis=1, keepdims=True)), jnp.exp(-new_m)
        )
        gated = numer / ((1.0 + jnp.exp(-out_pre)) * denom)
        head_ref[:, h * value_size : (h + 1) * value_size] = gated.astype(jnp.bfloat16)
    for store in stores:
        store.wait()


def tp_total(buf, send_sem, recv_sem):
    tp = lax.axis_index("tp")
    count = lax.axis_size("tp")
    copies = []
    for step in range(1, count):
        copy = remote("tp", step, buf.at[tp], buf.at[tp], send_sem.at[step], recv_sem.at[step])
        copy.start()
        copies.append(copy)
    for copy in copies:
        copy.wait_recv()
    total = buf[0].astype(jnp.float32)
    for i in range(1, count):
        total += buf[i].astype(jnp.float32)
    return total, copies


def rest_kernel(
    head_ref, tok_ref, gain_ref, wo, wg, wu, wd,
    mixed_ref,
    wo_v, wg_v, wu_v, wd_v, heads_all, abuf, dbuf, gpart, gland, upart, uland, spart, sland, hbuf,
    load_sem, hsend, hrecv, asend, arecv, dsend, drecv, esend, erecv, bsend, brecv,
):
    kv = lax.axis_index("kv")
    tp = lax.axis_index("tp")
    count = lax.axis_size("kv")
    batch, width = tok_ref.shape
    rows = batch // count
    loads = [
        pltpu.make_async_copy(src, dst, load_sem.at[i])
        for i, (src, dst) in enumerate([(wo, wo_v), (wg, wg_v), (wu, wu_v), (wd, wd_v)])
    ]
    barrier = pltpu.get_barrier_semaphore()
    signal_peers(barrier, "kv")
    signal_peers(barrier, "tp")
    for load in loads:
        load.start()
    pl.semaphore_wait(barrier, count - 1 + lax.axis_size("tp") - 1)
    gone = []
    arrive = []
    for step in range(1, count):
        copy = remote(
            "kv", step, head_ref, heads_all.at[kv], hsend.at[step], hrecv.at[step]
        )
        copy.start()
        arrive.append(copy)
    gone += arrive
    heads_all[kv] = head_ref[...]
    loads[0].wait()
    for copy in arrive:
        copy.wait_recv()
    heads = heads_all[...].astype(jnp.float32).reshape(batch, -1).astype(jnp.bfloat16)
    abuf[tp] = jnp.dot(heads, wo_v[...], preferred_element_type=jnp.float32).astype(jnp.bfloat16)
    attn_mix, copies = tp_total(abuf, asend, arecv)
    gone += copies
    middle = (tok_ref[...].astype(jnp.float32) + attn_mix).astype(jnp.bfloat16)
    mid = middle.astype(jnp.float32)
    squares = jnp.sum(mid * mid, axis=1, keepdims=True)
    normed = (mid * gain_ref[...]).astype(jnp.bfloat16)
    spart[...] = jnp.broadcast_to(squares, (batch, LANES)).reshape(count, rows, LANES)
    groups = []
    for i, (weight, part, land) in enumerate(
        [(None, spart, sland), (wg_v, gpart, gland), (wu_v, upart, uland)]
    ):
        if weight is not None:
            loads[i].wait()
            for off, size in pieces(weight.shape[0]):
                out = lax.dot_general(
                    normed, weight[off : off + size, :], (((1,), (1,)), ((), ())),
                    preferred_element_type=jnp.float32,
                )
                part[:, :, off : off + size] = out.reshape(count, rows, size).astype(jnp.bfloat16)
        group = []
        for step in range(1, count):
            copy = remote(
                "kv", step, part.at[peer_of("kv", step)], land.at[step],
                esend.at[i, step], erecv.at[i, step],
            )
            copy.start()
            group.append(copy)
        groups.append((part, land, group))
        gone += group
    sums = []
    for part, land, group in groups:
        for copy in group:
            copy.wait_recv()
        acc = part[kv].astype(jnp.float32)
        for step in range(1, count):
            acc += land[step].astype(jnp.float32)
        sums.append(acc)
    scale = lax.rsqrt(sums[0][:, :1] / (width * count) + norm_floor)
    gate = sums[1] * scale
    hidden = gate / (1.0 + jnp.exp(-gate)) * (sums[2] * scale)
    hbuf[kv] = hidden.astype(jnp.bfloat16)
    arrive = []
    for step in range(1, count):
        copy = remote("kv", step, hbuf.at[kv], hbuf.at[kv], bsend.at[step], brecv.at[step])
        copy.start()
        arrive.append(copy)
    gone += arrive
    loads[3].wait()
    for copy in arrive:
        copy.wait_recv()
    hid = hbuf[...].astype(jnp.float32).reshape(batch, -1).astype(jnp.bfloat16)
    dbuf[tp] = jnp.dot(hid, wd_v[...], preferred_element_type=jnp.float32).astype(jnp.bfloat16)
    down, copies = tp_total(dbuf, dsend, drecv)
    gone += copies
    mixed_ref[...] = (mid + down).astype(jnp.bfloat16)
    for copy in gone:
        copy.wait_send()


def per_device(
    tokens,
    attn_gain,
    w_query,
    w_key,
    w_value,
    w_outgate,
    w_gates,
    forget_bias,
    state_c,
    state_n,
    state_m,
    w_output,
    mlp_gain,
    w_gateff,
    w_upff,
    w_downff,
):
    f32, bf16 = jnp.float32, jnp.bfloat16
    count = lax.axis_size("kv")
    tps = lax.axis_size("tp")
    batch, width = tokens.shape
    rows, heads_dev, value_size, query_size = state_c.shape
    projections = (w_query, w_key, w_value, w_outgate)
    proj_width = sum(w.shape[1] for w in projections)
    hidden = w_gateff.shape[1]
    value_width = heads_dev * value_size
    rest_weights = (w_output, w_gateff.T, w_upff.T, w_downff)
    sem = pltpu.SemaphoreType.DMA
    struct = jax.ShapeDtypeStruct

    proj, gates = pl.pallas_call(
        project_kernel,
        out_shape=(struct((rows, proj_width), f32), struct((rows, LANES), f32)),
        in_specs=[VMEM_SPEC] * 2 + [HBM_SPEC] * 5,
        out_specs=(VMEM_SPEC, VMEM_SPEC),
        scratch_shapes=[pltpu.VMEM(w.shape, bf16) for w in projections]
        + [
            pltpu.VMEM((w_gates.shape[1], width), bf16),
            pltpu.VMEM((count, rows, proj_width), bf16),
            pltpu.VMEM((count, rows, proj_width), bf16),
            pltpu.VMEM((count, rows, LANES), f32),
            pltpu.VMEM((count, rows, LANES), f32),
            sem((5,)),
            sem((4, count)),
            sem((4, count)),
            sem((count,)),
            sem((count,)),
        ],
        compiler_params=pltpu.CompilerParams(
            collective_id=0, has_side_effects=True, vmem_limit_bytes=12 * 2**20
        ),
        name="project",
    )(tokens, attn_gain[None], w_query, w_key, w_value, w_outgate, w_gates.T)

    head_out, new_n, new_m, new_c = pl.pallas_call(
        state_kernel,
        out_shape=(
            struct((rows, value_width), bf16),
            struct(state_n.shape, f32),
            struct(state_m.shape, f32),
            struct(state_c.shape, f32),
        ),
        in_specs=[VMEM_SPEC] * 5 + [HBM_SPEC],
        out_specs=(VMEM_SPEC, VMEM_SPEC, VMEM_SPEC, HBM_SPEC),
        scratch_shapes=[
            pltpu.VMEM(state_c.shape, f32),
            sem((rows, heads_dev)),
            sem((rows, heads_dev)),
        ],
        compiler_params=pltpu.CompilerParams(vmem_limit_bytes=16 * 2**20),
        name="state",
    )(proj, gates, forget_bias[None], state_m, state_n, state_c)

    mixed = pl.pallas_call(
        rest_kernel,
        out_shape=struct((batch, width), bf16),
        in_specs=[VMEM_SPEC] * 3 + [HBM_SPEC] * 4,
        out_specs=VMEM_SPEC,
        scratch_shapes=[pltpu.VMEM(w.shape, bf16) for w in rest_weights]
        + [
            pltpu.VMEM((count, rows, value_width), bf16),
            pltpu.VMEM((tps, batch, width), bf16),
            pltpu.VMEM((tps, batch, width), bf16),
            pltpu.VMEM((count, rows, hidden), bf16),
            pltpu.VMEM((count, rows, hidden), bf16),
            pltpu.VMEM((count, rows, hidden), bf16),
            pltpu.VMEM((count, rows, hidden), bf16),
            pltpu.VMEM((count, rows, LANES), f32),
            pltpu.VMEM((count, rows, LANES), f32),
            pltpu.VMEM((count, rows, hidden), bf16),
            sem((4,)),
            sem((count,)),
            sem((count,)),
            sem((tps,)),
            sem((tps,)),
            sem((tps,)),
            sem((tps,)),
            sem((3, count)),
            sem((3, count)),
            sem((count,)),
            sem((count,)),
        ],
        compiler_params=pltpu.CompilerParams(
            collective_id=1, has_side_effects=True, vmem_limit_bytes=32 * 2**20
        ),
        name="rest",
    )(head_out, tokens, mlp_gain[None], *rest_weights)
    return (mixed, new_c, new_n, new_m)


def solution(mesh):
    placed = (
        P(None, "kv"),
        P("kv"),
        P("kv", "tp"),
        P("kv", "tp"),
        P("kv", "tp"),
        P("kv", "tp"),
        P(),
        P(),
        P("kv", "tp", None, None),
        P("kv", "tp", None),
        P("kv", "tp"),
        P("tp", "kv"),
        P("kv"),
        P("kv", "tp"),
        P("kv", "tp"),
        P("tp", "kv"),
    )
    return jax.shard_map(
        per_device,
        mesh=mesh,
        in_specs=placed,
        out_specs=(P(None, "kv"), P("kv", "tp", None, None), P("kv", "tp", None), P("kv", "tp")),
        check_vma=False,
    )
```

```python
import jax
import jax.numpy as jnp
from jax import lax
from jax.experimental import pallas as pl
from jax.experimental.pallas import tpu as pltpu
from jax.sharding import PartitionSpec as P

norm_floor = 1e-05
MESH = pl.DeviceIdType.MESH
LANES = 128
CHUNK = 512
SPANS = 4
VMEM_ALL = 67043328
SLACK = 640 * 1024
VMEM_SPEC = pl.BlockSpec(memory_space=pltpu.VMEM)
HBM_SPEC = pl.BlockSpec(memory_space=pltpu.HBM)


def pieces(total):
    return [(at, min(CHUNK, total - at)) for at in range(0, total, CHUNK)]


def peer_of(axis, step):
    count = lax.axis_size(axis)
    return lax.rem(lax.axis_index(axis) + step, count)


def signal_peers(barrier, axis):
    for step in range(1, lax.axis_size(axis)):
        pl.semaphore_signal(
            barrier, inc=1, device_id={axis: peer_of(axis, step)}, device_id_type=MESH
        )


def remote(axis, step, src, dst, send_sem, recv_sem):
    return pltpu.make_async_remote_copy(
        src_ref=src,
        dst_ref=dst,
        send_sem=send_sem,
        recv_sem=recv_sem,
        device_id={axis: peer_of(axis, step)},
        device_id_type=MESH,
    )


def inner_size(count):
    size = 1 << ((count.bit_length() - 1) // 2)
    return size if count % size == 0 else 1


def place():
    count = lax.axis_size("kv")
    inner = inner_size(count)
    kv = lax.axis_index("kv")
    return kv // inner, kv % inner, count // inner, inner


def inner_peer(step):
    outer_at, inner_at, _, inner = place()
    return (inner_at + step) % inner, outer_at * inner + (inner_at + step) % inner


def outer_peer(step):
    outer_at, inner_at, outer, inner = place()
    return (outer_at + step) % outer, ((outer_at + step) % outer) * inner + inner_at


def send_to(device, src, dst, send_sem, recv_sem):
    copy = pltpu.make_async_remote_copy(
        src_ref=src,
        dst_ref=dst,
        send_sem=send_sem,
        recv_sem=recv_sem,
        device_id={"kv": device},
        device_id_type=MESH,
    )
    copy.start()
    return copy


def scatter_first(i, part, land, columns, send_sem, recv_sem):
    _, _, _, inner = place()
    copies = []
    for step in range(1, inner):
        at, device = inner_peer(step)
        copies.append(
            send_to(
                device, part.at[at, :, :, columns], land.at[step, :, :, columns],
                send_sem.at[i, step], recv_sem.at[i, step],
            )
        )
    return copies


def scatter_second(i, first, part, land, both, last, at, size, send_sem, recv_sem):
    _, inner_at, outer, inner = place()
    columns = pl.ds(at, size)
    for copy in first:
        copy.wait_recv()
    acc = part[inner_at, :, :, at : at + size].astype(jnp.float32)
    for step in range(1, inner):
        acc += land[step, :, :, at : at + size].astype(jnp.float32)
    both[:, :, at : at + size] = acc.astype(jnp.bfloat16)
    copies = []
    for step in range(1, outer):
        to, device = outer_peer(step)
        copies.append(
            send_to(
                device, both.at[to, :, columns], last.at[step, :, columns],
                send_sem.at[i, step], recv_sem.at[i, step],
            )
        )
    return copies


def scatter_sum(second, both, last, at, size):
    outer_at, _, outer, _ = place()
    for copy in second:
        copy.wait_recv()
    acc = both[outer_at, :, at : at + size].astype(jnp.float32)
    for step in range(1, outer):
        acc += last[step, :, at : at + size].astype(jnp.float32)
    return acc


def put_part(part, out, at, size):
    inner, outer, rows, _ = part.shape
    split = out.reshape(outer, inner, rows, size).astype(jnp.bfloat16)
    for i in range(inner):
        part[i, :, :, at : at + size] = split[:, i]


def project_kernel(
    tok_ref, gain_ref, wq, wk, wv, wo, wg,
    proj_ref, gate_ref,
    wq_v, wk_v, wv_v, wo_v, wg_v, part, land, both, last, gpart, gland,
    load_sem, send_sem, recv_sem, send2_sem, recv2_sem, gsend_sem, grecv_sem,
):
    kv = lax.axis_index("kv")
    count = lax.axis_size("kv")
    batch, width = tok_ref.shape
    rows = batch // count
    weights = [(wq, wq_v), (wk, wk_v), (wv, wv_v), (wo, wo_v)]
    loads = [
        pltpu.make_async_copy(wg.at[:, pl.ds(pl.multiple_of(kv * width, LANES), width)], wg_v, load_sem.at[len(weights)])
    ]
    loads += [
        pltpu.make_async_copy(src, dst, load_sem.at[i]) for i, (src, dst) in enumerate(weights)
    ]
    barrier = pltpu.get_barrier_semaphore()
    signal_peers(barrier, "kv")
    for load in loads:
        load.start()
    tok = tok_ref[...].astype(jnp.float32)
    squares = jnp.sum(tok * tok, axis=1, keepdims=True)
    normed = (tok * gain_ref[...]).astype(jnp.bfloat16)
    loads[0].wait()
    gates = lax.dot_general(
        normed, wg_v[...], (((1,), (1,)), ((), ())), preferred_element_type=jnp.float32
    )
    gate_cols = gates.shape[1]
    gpart[...] = jnp.broadcast_to(squares, (batch, LANES)).reshape(count, rows, LANES)
    gpart[:, :, :gate_cols] = gates.reshape(count, rows, gate_cols)
    pl.semaphore_wait(barrier, count - 1)
    copies = []
    for step in range(1, count):
        copy = remote(
            "kv", step, gpart.at[peer_of("kv", step)], gland.at[step],
            gsend_sem.at[step], grecv_sem.at[step],
        )
        copy.start()
        copies.append(copy)
    at = 0
    groups = []
    for i, (_, dst) in enumerate(weights):
        loads[i + 1].wait()
        wide = dst.shape[1]
        for off, size in pieces(wide):
            out = jnp.dot(normed, dst[:, off : off + size], preferred_element_type=jnp.float32)
            put_part(part, out, at + off, size)
        copies_one = scatter_first(i, part, land, pl.ds(at, wide), send_sem, recv_sem)
        groups.append((at, wide, copies_one))
        at += wide
    seconds = [
        scatter_second(i, first, part, land, both, last, at, wide, send2_sem, recv2_sem)
        for i, (at, wide, first) in enumerate(groups)
    ]
    total = gpart[kv]
    for copy in copies:
        copy.wait_recv()
    for step in range(1, count):
        total += gland[step]
    mean = total[:, gate_cols : gate_cols + 1] / (width * count)
    scale = lax.rsqrt(mean + norm_floor)
    gate_ref[...] = total * scale
    for (at, wide, _), second in zip(groups, seconds):
        proj_ref[:, at : at + wide] = scatter_sum(second, both, last, at, wide) * scale
    for copy in copies:
        copy.wait_send()
    for (_, _, first), second in zip(groups, seconds):
        for copy in first + second:
            copy.wait_send()


def state_kernel(
    proj_ref, gate_ref, bias_ref, m_ref, n_ref, c_hbm,
    head_ref, newn_ref, newm_ref, newc_hbm,
    held, in_sem, out_sem,
):
    rows, heads, value_size, query_size = held.shape
    tp = lax.axis_index("tp")
    heads_all = bias_ref.shape[1]
    loads = [
        pltpu.make_async_copy(c_hbm.at[b, h], held.at[b, h], in_sem.at[b, h])
        for h in range(heads)
        for b in range(rows)
    ]
    for load in loads:
        load.start()
    gates = gate_ref[...]
    lane = lax.broadcasted_iota(jnp.int32, gates.shape, 1)
    bias_lane = lax.broadcasted_iota(jnp.int32, bias_ref.shape, 1)
    sub = lax.broadcasted_iota(jnp.int32, (rows, value_size), 0)
    query_width = heads * query_size
    value_at = 2 * query_width
    out_at = value_at + heads * value_size
    stores = []
    for h in range(heads):
        column = tp * heads + h
        log_input = jnp.sum(jnp.where(lane == column, gates, 0.0), axis=1, keepdims=True)
        forget = jnp.sum(jnp.where(lane == heads_all + column, gates, 0.0), axis=1, keepdims=True)
        bias = jnp.sum(jnp.where(bias_lane == column, bias_ref[...], 0.0), axis=1, keepdims=True)
        pre = forget + bias
        log_forget = jnp.minimum(pre, 0.0) - jnp.log(1.0 + jnp.exp(-jnp.abs(pre)))
        carried = log_forget + m_ref[:, h : h + 1]
        new_m = jnp.maximum(carried, log_input)
        keep = jnp.exp(carried - new_m)
        admit = jnp.exp(log_input - new_m)
        newm_ref[:, h : h + 1] = new_m
        query = proj_ref[:, h * query_size : (h + 1) * query_size] * query_size ** (-0.5)
        key_at = query_width + h * query_size
        key = admit * proj_ref[:, key_at : key_at + query_size]
        v_at = value_at + h * value_size
        value = proj_ref[:, v_at : v_at + value_size]
        o_at = out_at + h * value_size
        out_pre = proj_ref[:, o_at : o_at + value_size]
        new_n = keep * n_ref[:, h, :] + key
        newn_ref[:, h, :] = new_n
        value_cols = value.T
        keep_wide = jnp.broadcast_to(keep, (rows, query_size))
        query_low = query.astype(jnp.bfloat16)
        read = jnp.zeros((rows, value_size), jnp.float32)
        for b in range(rows):
            loads[h * rows + b].wait()
            old = held[b, h]
            one = lax.dot_general(
                query_low, old.astype(jnp.bfloat16), (((1,), (1,)), ((), ())),
                preferred_element_type=jnp.float32,
            )
            read = jnp.where(sub == b, one, read)
            held[b, h] = (
                keep_wide[b : b + 1, :] * old + value_cols[:, b : b + 1] * key[b : b + 1, :]
            )
            store = pltpu.make_async_copy(held.at[b, h], newc_hbm.at[b, h], out_sem.at[b, h])
            store.start()
            stores.append(store)
        numer = keep * read + value * jnp.sum(key * query, axis=1, keepdims=True)
        denom = jnp.maximum(
            jnp.abs(jnp.sum(new_n * query, axis=1, keepdims=True)), jnp.exp(-new_m)
        )
        gated = numer / ((1.0 + jnp.exp(-out_pre)) * denom)
        head_ref[:, h * value_size : (h + 1) * value_size] = gated.astype(jnp.bfloat16)
    for store in stores:
        store.wait()


def hidden_spans(hidden):
    wide = -(-hidden // (SPANS * LANES)) * LANES
    return [(at, min(wide, hidden - at)) for at in range(0, hidden, wide)]


def tp_total(buf, send_sem, recv_sem):
    tp = lax.axis_index("tp")
    count = lax.axis_size("tp")
    copies = []
    for step in range(1, count):
        copy = remote("tp", step, buf.at[tp], buf.at[tp], send_sem.at[step], recv_sem.at[step])
        copy.start()
        copies.append(copy)
    for copy in copies:
        copy.wait_recv()
    total = buf[0].astype(jnp.float32)
    for i in range(1, count):
        total += buf[i].astype(jnp.float32)
    return total, copies


def rest_kernel(
    head_ref, tok_ref, gain_ref, wo, wg, wu, wd,
    mixed_ref,
    wo_v, wg_v, wu_v, wd_v, heads_all, abuf, dbuf, gpart, gland, gboth, glast,
    upart, uland, uboth, ulast, spart, sland, hbuf,
    load_sem, hsend, hrecv, asend, arecv, dsend, drecv, ssend, srecv, esend, erecv, fsend, frecv,
    bsend, brecv, csend, crecv,
):
    kv = lax.axis_index("kv")
    tp = lax.axis_index("tp")
    count = lax.axis_size("kv")
    batch, width = tok_ref.shape
    rows = batch // count
    loads = [
        pltpu.make_async_copy(src, dst, load_sem.at[i])
        for i, (src, dst) in enumerate([(wo, wo_v), (wg, wg_v), (wu, wu_v), (wd, wd_v)])
    ]
    barrier = pltpu.get_barrier_semaphore()
    signal_peers(barrier, "kv")
    signal_peers(barrier, "tp")
    for load in loads:
        load.start()
    pl.semaphore_wait(barrier, count - 1 + lax.axis_size("tp") - 1)
    gone = []
    arrive = []
    for step in range(1, count):
        copy = remote(
            "kv", step, head_ref, heads_all.at[kv], hsend.at[step], hrecv.at[step]
        )
        copy.start()
        arrive.append(copy)
    gone += arrive
    heads_all[kv] = head_ref[...]
    loads[0].wait()
    for copy in arrive:
        copy.wait_recv()
    heads = heads_all[...].astype(jnp.float32).reshape(batch, -1).astype(jnp.bfloat16)
    abuf[tp] = jnp.dot(heads, wo_v[...], preferred_element_type=jnp.float32).astype(jnp.bfloat16)
    attn_mix, copies = tp_total(abuf, asend, arecv)
    gone += copies
    middle = (tok_ref[...].astype(jnp.float32) + attn_mix).astype(jnp.bfloat16)
    mid = middle.astype(jnp.float32)
    squares = jnp.sum(mid * mid, axis=1, keepdims=True)
    normed = (mid * gain_ref[...]).astype(jnp.bfloat16)
    spart[...] = jnp.broadcast_to(squares, (batch, LANES)).reshape(count, rows, LANES)
    square_copies = [
        send_to(
            peer_of("kv", step), spart.at[peer_of("kv", step)], sland.at[step],
            ssend.at[step], srecv.at[step],
        )
        for step in range(1, count)
    ]
    gone += square_copies
    hidden = wg_v.shape[0]
    spans = hidden_spans(hidden)
    groups = []
    for w, (weight, part, land, both, last) in enumerate(
        [(wg_v, gpart, gland, gboth, glast), (wu_v, upart, uland, uboth, ulast)]
    ):
        loads[w + 1].wait()
        for k, (at, wide) in enumerate(spans):
            for off, size in pieces(wide):
                out = lax.dot_general(
                    normed, weight[at + off : at + off + size, :], (((1,), (1,)), ((), ())),
                    preferred_element_type=jnp.float32,
                )
                put_part(part, out, at + off, size)
            i = w * len(spans) + k
            first = scatter_first(i, part, land, pl.ds(at, wide), esend, erecv)
            groups.append((i, first, part, land, both, last, at, wide))
            gone += first
    seconds = [scatter_second(*group, fsend, frecv) for group in groups]
    for second in seconds:
        gone += second
    for copy in square_copies:
        copy.wait_recv()
    total = spart[kv]
    for step in range(1, count):
        total += sland[step]
    scale = lax.rsqrt(total[:, :1] / (width * count) + norm_floor)
    outer_at, inner_at, outer, inner = place()
    for k, (at, wide) in enumerate(spans):
        gate = scatter_sum(seconds[k], gboth, glast, at, wide) * scale
        up = scatter_sum(seconds[k + len(spans)], uboth, ulast, at, wide) * scale
        hid = gate / (1.0 + jnp.exp(-gate)) * up
        hbuf[outer_at, inner_at, :, at : at + wide] = hid.astype(jnp.bfloat16)
    own = hbuf.at[outer_at, inner_at]
    along = [
        send_to(outer_peer(step)[1], own, own, bsend.at[step], brecv.at[step])
        for step in range(1, outer)
    ]
    across = []
    for far in range(outer):
        if far > 0:
            along[far - 1].wait_recv()
        block = hbuf.at[(outer_at + outer - far) % outer, inner_at]
        for step in range(1, inner):
            across.append(
                send_to(inner_peer(step)[1], block, block, csend.at[far, step], crecv.at[far, step])
            )
    arrive = across
    gone += along + across
    loads[3].wait()
    for copy in arrive:
        copy.wait_recv()
    hid = hbuf[...].astype(jnp.float32).reshape(batch, -1).astype(jnp.bfloat16)
    dbuf[tp] = jnp.dot(hid, wd_v[...], preferred_element_type=jnp.float32).astype(jnp.bfloat16)
    down, copies = tp_total(dbuf, dsend, drecv)
    gone += copies
    mixed_ref[...] = (mid + down).astype(jnp.bfloat16)
    for copy in gone:
        copy.wait_send()


def per_device(
    tokens,
    attn_gain,
    w_query,
    w_key,
    w_value,
    w_outgate,
    w_gates,
    forget_bias,
    state_c,
    state_n,
    state_m,
    w_output,
    mlp_gain,
    w_gateff,
    w_upff,
    w_downff,
):
    f32, bf16 = jnp.float32, jnp.bfloat16
    count = lax.axis_size("kv")
    tps = lax.axis_size("tp")
    batch, width = tokens.shape
    rows, heads_dev, value_size, query_size = state_c.shape
    projections = (w_query, w_key, w_value, w_outgate)
    proj_width = sum(w.shape[1] for w in projections)
    hidden = w_gateff.shape[1]
    value_width = heads_dev * value_size
    rest_weights = (w_output, w_gateff.T, w_upff.T, w_downff)
    inner = inner_size(count)
    outer = count // inner
    spans = len(hidden_spans(hidden))
    sem = pltpu.SemaphoreType.DMA
    struct = jax.ShapeDtypeStruct

    proj, gates = pl.pallas_call(
        project_kernel,
        out_shape=(
            struct((rows, proj_width), f32),
            struct((rows, LANES), f32),
        ),
        in_specs=[VMEM_SPEC] * 2 + [HBM_SPEC] * 5,
        out_specs=(VMEM_SPEC, VMEM_SPEC),
        scratch_shapes=[pltpu.VMEM(w.shape, bf16) for w in projections]
        + [
            pltpu.VMEM((w_gates.shape[1], width), bf16),
            pltpu.VMEM((inner, outer, rows, proj_width), bf16),
            pltpu.VMEM((inner, outer, rows, proj_width), bf16),
            pltpu.VMEM((outer, rows, proj_width), bf16),
            pltpu.VMEM((outer, rows, proj_width), bf16),
            pltpu.VMEM((count, rows, LANES), f32),
            pltpu.VMEM((count, rows, LANES), f32),
            sem((5,)),
            sem((4, inner)),
            sem((4, inner)),
            sem((4, outer)),
            sem((4, outer)),
            sem((count,)),
            sem((count,)),
        ],
        compiler_params=pltpu.CompilerParams(
            collective_id=0, has_side_effects=True,
            vmem_limit_bytes=VMEM_ALL - SLACK,
        ),
        name="project",
    )(tokens, attn_gain[None], w_query, w_key, w_value, w_outgate, w_gates.T)

    head_out, new_n, new_m, new_c = pl.pallas_call(
        state_kernel,
        out_shape=(
            struct((rows, value_width), bf16),
            struct(state_n.shape, f32),
            struct(state_m.shape, f32),
            struct(state_c.shape, f32),
        ),
        in_specs=[VMEM_SPEC] * 5 + [HBM_SPEC],
        out_specs=(VMEM_SPEC, VMEM_SPEC, VMEM_SPEC, HBM_SPEC),
        scratch_shapes=[
            pltpu.VMEM(state_c.shape, f32),
            sem((rows, heads_dev)),
            sem((rows, heads_dev)),
        ],
        compiler_params=pltpu.CompilerParams(vmem_limit_bytes=VMEM_ALL - SLACK),
        name="state",
    )(proj, gates, forget_bias[None], state_m, state_n, state_c)

    mixed = pl.pallas_call(
        rest_kernel,
        out_shape=struct((batch, width), bf16),
        in_specs=[VMEM_SPEC] * 3 + [HBM_SPEC] * 4,
        out_specs=VMEM_SPEC,
        scratch_shapes=[pltpu.VMEM(w.shape, bf16) for w in rest_weights]
        + [
            pltpu.VMEM((count, rows, value_width), bf16),
            pltpu.VMEM((tps, batch, width), bf16),
            pltpu.VMEM((tps, batch, width), bf16),
        ]
        + [
            pltpu.VMEM((inner, outer, rows, hidden), bf16),
            pltpu.VMEM((inner, outer, rows, hidden), bf16),
            pltpu.VMEM((outer, rows, hidden), bf16),
            pltpu.VMEM((outer, rows, hidden), bf16),
        ]
        * 2
        + [
            pltpu.VMEM((count, rows, LANES), f32),
            pltpu.VMEM((count, rows, LANES), f32),
            pltpu.VMEM((outer, inner, rows, hidden), bf16),
            sem((4,)),
            sem((count,)),
            sem((count,)),
            sem((tps,)),
            sem((tps,)),
            sem((tps,)),
            sem((tps,)),
            sem((count,)),
            sem((count,)),
            sem((2 * spans, inner)),
            sem((2 * spans, inner)),
            sem((2 * spans, outer)),
            sem((2 * spans, outer)),
            sem((outer,)),
            sem((outer,)),
            sem((outer, inner)),
            sem((outer, inner)),
        ],
        compiler_params=pltpu.CompilerParams(
            collective_id=1, has_side_effects=True, vmem_limit_bytes=VMEM_ALL - SLACK
        ),
        name="rest",
    )(head_out, tokens, mlp_gain[None], *rest_weights)
    return (mixed, new_c, new_n, new_m)


def solution(mesh):
    placed = (
        P(None, "kv"),
        P("kv"),
        P("kv", "tp"),
        P("kv", "tp"),
        P("kv", "tp"),
        P("kv", "tp"),
        P(),
        P(),
        P("kv", "tp", None, None),
        P("kv", "tp", None),
        P("kv", "tp"),
        P("tp", "kv"),
        P("kv"),
        P("kv", "tp"),
        P("kv", "tp"),
        P("tp", "kv"),
    )
    return jax.shard_map(
        per_device,
        mesh=mesh,
        in_specs=placed,
        out_specs=(P(None, "kv"), P("kv", "tp", None, None), P("kv", "tp", None), P("kv", "tp")),
        check_vma=False,
    )
```

```python
import jax
import jax.numpy as jnp
from jax import lax
from jax.experimental import pallas as pl
from jax.experimental.pallas import tpu as pltpu
from jax.sharding import PartitionSpec as P

norm_floor = 1e-05
MESH = pl.DeviceIdType.MESH
LANES = 128
CHUNK = 512
SPANS = 4
VMEM_ALL = 67043328
SLACK = 640 * 1024
VMEM_SPEC = pl.BlockSpec(memory_space=pltpu.VMEM)
HBM_SPEC = pl.BlockSpec(memory_space=pltpu.HBM)


def pieces(total):
    return [(at, min(CHUNK, total - at)) for at in range(0, total, CHUNK)]


def peer_of(axis, step):
    count = lax.axis_size(axis)
    return lax.rem(lax.axis_index(axis) + step, count)


def signal_peers(barrier, axis):
    for step in range(1, lax.axis_size(axis)):
        pl.semaphore_signal(
            barrier, inc=1, device_id={axis: peer_of(axis, step)}, device_id_type=MESH
        )


def remote(axis, step, src, dst, send_sem, recv_sem):
    return pltpu.make_async_remote_copy(
        src_ref=src,
        dst_ref=dst,
        send_sem=send_sem,
        recv_sem=recv_sem,
        device_id={axis: peer_of(axis, step)},
        device_id_type=MESH,
    )


def inner_size(count):
    size = 1 << ((count.bit_length() - 1) // 2)
    return size if count % size == 0 else 1


def place():
    count = lax.axis_size("kv")
    inner = inner_size(count)
    kv = lax.axis_index("kv")
    return kv // inner, kv % inner, count // inner, inner


def inner_peer(step):
    outer_at, inner_at, _, inner = place()
    return (inner_at + step) % inner, outer_at * inner + (inner_at + step) % inner


def outer_peer(step):
    outer_at, inner_at, outer, inner = place()
    return (outer_at + step) % outer, ((outer_at + step) % outer) * inner + inner_at


def send_to(device, src, dst, send_sem, recv_sem):
    copy = pltpu.make_async_remote_copy(
        src_ref=src,
        dst_ref=dst,
        send_sem=send_sem,
        recv_sem=recv_sem,
        device_id={"kv": device},
        device_id_type=MESH,
    )
    copy.start()
    return copy


def scatter_first(i, part, land, columns, send_sem, recv_sem):
    _, _, _, inner = place()
    copies = []
    for step in range(1, inner):
        at, device = inner_peer(step)
        copies.append(
            send_to(
                device, part.at[at, :, :, columns], land.at[step, :, :, columns],
                send_sem.at[i, step], recv_sem.at[i, step],
            )
        )
    return copies


def scatter_second(i, first, part, land, both, last, at, size, send_sem, recv_sem):
    _, inner_at, outer, inner = place()
    columns = pl.ds(at, size)
    for copy in first:
        copy.wait_recv()
    acc = part[inner_at, :, :, at : at + size].astype(jnp.float32)
    for step in range(1, inner):
        acc += land[step, :, :, at : at + size].astype(jnp.float32)
    both[:, :, at : at + size] = acc.astype(jnp.bfloat16)
    copies = []
    for step in range(1, outer):
        to, device = outer_peer(step)
        copies.append(
            send_to(
                device, both.at[to, :, columns], last.at[step, :, columns],
                send_sem.at[i, step], recv_sem.at[i, step],
            )
        )
    return copies


def scatter_sum(second, both, last, at, size):
    outer_at, _, outer, _ = place()
    for copy in second:
        copy.wait_recv()
    acc = both[outer_at, :, at : at + size].astype(jnp.float32)
    for step in range(1, outer):
        acc += last[step, :, at : at + size].astype(jnp.float32)
    return acc


def put_part(part, out, at, size):
    inner, outer, rows, _ = part.shape
    split = out.reshape(outer, inner, rows, size).astype(jnp.bfloat16)
    for i in range(inner):
        part[i, :, :, at : at + size] = split[:, i]


def project_kernel(
    tok_ref, gain_ref, wq, wk, wv, wo, wg,
    proj_ref, gate_ref,
    wq_v, wk_v, wv_v, wo_v, wg_v, part, land, both, last, gpart, gland,
    load_sem, send_sem, recv_sem, send2_sem, recv2_sem, gsend_sem, grecv_sem,
):
    kv = lax.axis_index("kv")
    count = lax.axis_size("kv")
    batch, width = tok_ref.shape
    rows = batch // count
    weights = [(wq, wq_v), (wk, wk_v), (wv, wv_v), (wo, wo_v)]
    loads = [
        pltpu.make_async_copy(wg.at[:, pl.ds(pl.multiple_of(kv * width, LANES), width)], wg_v, load_sem.at[len(weights)])
    ]
    loads += [
        pltpu.make_async_copy(src, dst, load_sem.at[i]) for i, (src, dst) in enumerate(weights)
    ]
    barrier = pltpu.get_barrier_semaphore()
    signal_peers(barrier, "kv")
    for load in loads:
        load.start()
    tok = tok_ref[...].astype(jnp.float32)
    squares = jnp.sum(tok * tok, axis=1, keepdims=True)
    normed = (tok * gain_ref[...]).astype(jnp.bfloat16)
    loads[0].wait()
    gates = lax.dot_general(
        normed, wg_v[...], (((1,), (1,)), ((), ())), preferred_element_type=jnp.float32
    )
    gate_cols = gates.shape[1]
    gpart[...] = jnp.broadcast_to(squares, (batch, LANES)).reshape(count, rows, LANES)
    gpart[:, :, :gate_cols] = gates.reshape(count, rows, gate_cols)
    pl.semaphore_wait(barrier, count - 1)
    copies = []
    for step in range(1, count):
        copy = remote(
            "kv", step, gpart.at[peer_of("kv", step)], gland.at[step],
            gsend_sem.at[step], grecv_sem.at[step],
        )
        copy.start()
        copies.append(copy)
    at = 0
    groups = []
    for i, (_, dst) in enumerate(weights):
        loads[i + 1].wait()
        wide = dst.shape[1]
        for off, size in pieces(wide):
            out = jnp.dot(normed, dst[:, off : off + size], preferred_element_type=jnp.float32)
            put_part(part, out, at + off, size)
        copies_one = scatter_first(i, part, land, pl.ds(at, wide), send_sem, recv_sem)
        groups.append((at, wide, copies_one))
        at += wide
    seconds = [
        scatter_second(i, first, part, land, both, last, at, wide, send2_sem, recv2_sem)
        for i, (at, wide, first) in enumerate(groups)
    ]
    total = gpart[kv]
    for copy in copies:
        copy.wait_recv()
    for step in range(1, count):
        total += gland[step]
    mean = total[:, gate_cols : gate_cols + 1] / (width * count)
    scale = lax.rsqrt(mean + norm_floor)
    gate_ref[...] = total * scale
    for (at, wide, _), second in zip(groups, seconds):
        proj_ref[:, at : at + wide] = scatter_sum(second, both, last, at, wide) * scale
    for copy in copies:
        copy.wait_send()
    for (_, _, first), second in zip(groups, seconds):
        for copy in first + second:
            copy.wait_send()


def state_kernel(
    proj_ref, gate_ref, bias_ref, m_ref, n_ref, c_hbm,
    head_ref, newn_ref, newm_ref, newc_hbm,
    held, in_sem, out_sem,
):
    rows, heads, value_size, query_size = held.shape
    tp = lax.axis_index("tp")
    heads_all = bias_ref.shape[1]
    loads = [
        pltpu.make_async_copy(c_hbm.at[b, h], held.at[b, h], in_sem.at[b, h])
        for h in range(heads)
        for b in range(rows)
    ]
    for load in loads:
        load.start()
    gates = gate_ref[...]
    lane = lax.broadcasted_iota(jnp.int32, gates.shape, 1)
    bias_lane = lax.broadcasted_iota(jnp.int32, bias_ref.shape, 1)
    sub = lax.broadcasted_iota(jnp.int32, (rows, value_size), 0)
    eye = lax.broadcasted_iota(jnp.int32, (rows, rows), 0) == lax.broadcasted_iota(
        jnp.int32, (rows, rows), 1
    )
    query_width = heads * query_size
    value_at = 2 * query_width
    out_at = value_at + heads * value_size
    stores = []
    for h in range(heads):
        column = tp * heads + h
        log_input = jnp.sum(jnp.where(lane == column, gates, 0.0), axis=1, keepdims=True)
        forget = jnp.sum(jnp.where(lane == heads_all + column, gates, 0.0), axis=1, keepdims=True)
        bias = jnp.sum(jnp.where(bias_lane == column, bias_ref[...], 0.0), axis=1, keepdims=True)
        pre = forget + bias
        log_forget = jnp.minimum(pre, 0.0) - jnp.log(1.0 + jnp.exp(-jnp.abs(pre)))
        old_m = jnp.sum(jnp.where(eye, m_ref[h : h + 1, :], 0.0), axis=1, keepdims=True)
        carried = log_forget + old_m
        new_m = jnp.maximum(carried, log_input)
        keep = jnp.exp(carried - new_m)
        admit = jnp.exp(log_input - new_m)
        newm_ref[h : h + 1, :] = jnp.sum(jnp.where(eye, new_m, 0.0), axis=0, keepdims=True)
        query = proj_ref[:, h * query_size : (h + 1) * query_size] * query_size ** (-0.5)
        key_at = query_width + h * query_size
        key = admit * proj_ref[:, key_at : key_at + query_size]
        v_at = value_at + h * value_size
        value = proj_ref[:, v_at : v_at + value_size]
        o_at = out_at + h * value_size
        out_pre = proj_ref[:, o_at : o_at + value_size]
        new_n = keep * n_ref[:, h, :] + key
        newn_ref[:, h, :] = new_n
        value_cols = value.T
        keep_wide = jnp.broadcast_to(keep, (rows, query_size))
        query_low = query.astype(jnp.bfloat16)
        read = jnp.zeros((rows, value_size), jnp.float32)
        for b in range(rows):
            loads[h * rows + b].wait()
            old = held[b, h]
            one = lax.dot_general(
                query_low, old.astype(jnp.bfloat16), (((1,), (1,)), ((), ())),
                preferred_element_type=jnp.float32,
            )
            read = jnp.where(sub == b, one, read)
            held[b, h] = (
                keep_wide[b : b + 1, :] * old + value_cols[:, b : b + 1] * key[b : b + 1, :]
            )
            store = pltpu.make_async_copy(held.at[b, h], newc_hbm.at[b, h], out_sem.at[b, h])
            store.start()
            stores.append(store)
        numer = keep * read + value * jnp.sum(key * query, axis=1, keepdims=True)
        denom = jnp.maximum(
            jnp.abs(jnp.sum(new_n * query, axis=1, keepdims=True)), jnp.exp(-new_m)
        )
        gated = numer / ((1.0 + jnp.exp(-out_pre)) * denom)
        head_ref[:, h * value_size : (h + 1) * value_size] = gated.astype(jnp.bfloat16)
    for store in stores:
        store.wait()


def hidden_spans(hidden):
    wide = -(-hidden // (SPANS * LANES)) * LANES
    return [(at, min(wide, hidden - at)) for at in range(0, hidden, wide)]


def tp_total(buf, send_sem, recv_sem):
    tp = lax.axis_index("tp")
    count = lax.axis_size("tp")
    copies = []
    for step in range(1, count):
        copy = remote("tp", step, buf.at[tp], buf.at[tp], send_sem.at[step], recv_sem.at[step])
        copy.start()
        copies.append(copy)
    for copy in copies:
        copy.wait_recv()
    total = buf[0].astype(jnp.float32)
    for i in range(1, count):
        total += buf[i].astype(jnp.float32)
    return total, copies


def rest_kernel(
    head_ref, tok_ref, gain_ref, wo, wg, wu, wd,
    mixed_ref,
    wo_v, wg_v, wu_v, wd_v, heads_all, abuf, dbuf, gpart, gland, gboth, glast,
    upart, uland, uboth, ulast, spart, sland, hbuf,
    load_sem, hsend, hrecv, asend, arecv, dsend, drecv, ssend, srecv, esend, erecv, fsend, frecv,
    bsend, brecv, csend, crecv,
):
    kv = lax.axis_index("kv")
    tp = lax.axis_index("tp")
    count = lax.axis_size("kv")
    batch, width = tok_ref.shape
    rows = batch // count
    loads = [
        pltpu.make_async_copy(src, dst, load_sem.at[i])
        for i, (src, dst) in enumerate([(wo, wo_v), (wg, wg_v), (wu, wu_v), (wd, wd_v)])
    ]
    barrier = pltpu.get_barrier_semaphore()
    signal_peers(barrier, "kv")
    signal_peers(barrier, "tp")
    for load in loads:
        load.start()
    pl.semaphore_wait(barrier, count - 1 + lax.axis_size("tp") - 1)
    gone = []
    arrive = []
    for step in range(1, count):
        copy = remote(
            "kv", step, head_ref, heads_all.at[kv], hsend.at[step], hrecv.at[step]
        )
        copy.start()
        arrive.append(copy)
    gone += arrive
    heads_all[kv] = head_ref[...]
    loads[0].wait()
    for copy in arrive:
        copy.wait_recv()
    heads = heads_all[...].astype(jnp.float32).reshape(batch, -1).astype(jnp.bfloat16)
    abuf[tp] = jnp.dot(heads, wo_v[...], preferred_element_type=jnp.float32).astype(jnp.bfloat16)
    attn_mix, copies = tp_total(abuf, asend, arecv)
    gone += copies
    middle = (tok_ref[...].astype(jnp.float32) + attn_mix).astype(jnp.bfloat16)
    mid = middle.astype(jnp.float32)
    squares = jnp.sum(mid * mid, axis=1, keepdims=True)
    normed = (mid * gain_ref[...]).astype(jnp.bfloat16)
    spart[...] = jnp.broadcast_to(squares, (batch, LANES)).reshape(count, rows, LANES)
    square_copies = [
        send_to(
            peer_of("kv", step), spart.at[peer_of("kv", step)], sland.at[step],
            ssend.at[step], srecv.at[step],
        )
        for step in range(1, count)
    ]
    gone += square_copies
    hidden = wg_v.shape[0]
    spans = hidden_spans(hidden)
    groups = []
    for w, (weight, part, land, both, last) in enumerate(
        [(wg_v, gpart, gland, gboth, glast), (wu_v, upart, uland, uboth, ulast)]
    ):
        loads[w + 1].wait()
        for k, (at, wide) in enumerate(spans):
            for off, size in pieces(wide):
                out = lax.dot_general(
                    normed, weight[at + off : at + off + size, :], (((1,), (1,)), ((), ())),
                    preferred_element_type=jnp.float32,
                )
                put_part(part, out, at + off, size)
            i = w * len(spans) + k
            first = scatter_first(i, part, land, pl.ds(at, wide), esend, erecv)
            groups.append((i, first, part, land, both, last, at, wide))
            gone += first
    seconds = [scatter_second(*group, fsend, frecv) for group in groups]
    for second in seconds:
        gone += second
    for copy in square_copies:
        copy.wait_recv()
    total = spart[kv]
    for step in range(1, count):
        total += sland[step]
    scale = lax.rsqrt(total[:, :1] / (width * count) + norm_floor)
    outer_at, inner_at, outer, inner = place()
    for k, (at, wide) in enumerate(spans):
        gate = scatter_sum(seconds[k], gboth, glast, at, wide) * scale
        up = scatter_sum(seconds[k + len(spans)], uboth, ulast, at, wide) * scale
        hid = gate / (1.0 + jnp.exp(-gate)) * up
        hbuf[outer_at, inner_at, :, at : at + wide] = hid.astype(jnp.bfloat16)
    own = hbuf.at[outer_at, inner_at]
    along = [
        send_to(outer_peer(step)[1], own, own, bsend.at[step], brecv.at[step])
        for step in range(1, outer)
    ]
    across = []
    for far in range(outer):
        if far > 0:
            along[far - 1].wait_recv()
        block = hbuf.at[(outer_at + outer - far) % outer, inner_at]
        for step in range(1, inner):
            across.append(
                send_to(inner_peer(step)[1], block, block, csend.at[far, step], crecv.at[far, step])
            )
    arrive = across
    gone += along + across
    loads[3].wait()
    for copy in arrive:
        copy.wait_recv()
    hid = hbuf[...].astype(jnp.float32).reshape(batch, -1).astype(jnp.bfloat16)
    dbuf[tp] = jnp.dot(hid, wd_v[...], preferred_element_type=jnp.float32).astype(jnp.bfloat16)
    down, copies = tp_total(dbuf, dsend, drecv)
    gone += copies
    mixed_ref[...] = (mid + down).astype(jnp.bfloat16)
    for copy in gone:
        copy.wait_send()


def per_device(
    tokens,
    attn_gain,
    w_query,
    w_key,
    w_value,
    w_outgate,
    w_gates,
    forget_bias,
    state_c,
    state_n,
    state_m,
    w_output,
    mlp_gain,
    w_gateff,
    w_upff,
    w_downff,
):
    f32, bf16 = jnp.float32, jnp.bfloat16
    count = lax.axis_size("kv")
    tps = lax.axis_size("tp")
    batch, width = tokens.shape
    rows, heads_dev, value_size, query_size = state_c.shape
    projections = (w_query, w_key, w_value, w_outgate)
    proj_width = sum(w.shape[1] for w in projections)
    hidden = w_gateff.shape[1]
    value_width = heads_dev * value_size
    rest_weights = (w_output, w_gateff.T, w_upff.T, w_downff)
    inner = inner_size(count)
    outer = count // inner
    spans = len(hidden_spans(hidden))
    sem = pltpu.SemaphoreType.DMA
    struct = jax.ShapeDtypeStruct

    proj, gates = pl.pallas_call(
        project_kernel,
        out_shape=(
            struct((rows, proj_width), f32),
            struct((rows, LANES), f32),
        ),
        in_specs=[VMEM_SPEC] * 2 + [HBM_SPEC] * 5,
        out_specs=(VMEM_SPEC, VMEM_SPEC),
        scratch_shapes=[pltpu.VMEM(w.shape, bf16) for w in projections]
        + [
            pltpu.VMEM((w_gates.shape[1], width), bf16),
            pltpu.VMEM((inner, outer, rows, proj_width), bf16),
            pltpu.VMEM((inner, outer, rows, proj_width), bf16),
            pltpu.VMEM((outer, rows, proj_width), bf16),
            pltpu.VMEM((outer, rows, proj_width), bf16),
            pltpu.VMEM((count, rows, LANES), f32),
            pltpu.VMEM((count, rows, LANES), f32),
            sem((5,)),
            sem((4, inner)),
            sem((4, inner)),
            sem((4, outer)),
            sem((4, outer)),
            sem((count,)),
            sem((count,)),
        ],
        compiler_params=pltpu.CompilerParams(
            collective_id=0, has_side_effects=True,
            vmem_limit_bytes=VMEM_ALL - SLACK,
        ),
        name="project",
    )(tokens, attn_gain[None], w_query, w_key, w_value, w_outgate, w_gates.T)

    head_out, new_n, new_m, new_c = pl.pallas_call(
        state_kernel,
        out_shape=(
            struct((rows, value_width), bf16),
            struct(state_n.shape, f32),
            struct(state_m.T.shape, f32),
            struct(state_c.shape, f32),
        ),
        in_specs=[VMEM_SPEC] * 5 + [HBM_SPEC],
        out_specs=(VMEM_SPEC, VMEM_SPEC, VMEM_SPEC, HBM_SPEC),
        scratch_shapes=[
            pltpu.VMEM(state_c.shape, f32),
            sem((rows, heads_dev)),
            sem((rows, heads_dev)),
        ],
        compiler_params=pltpu.CompilerParams(vmem_limit_bytes=VMEM_ALL - SLACK),
        name="state",
    )(proj, gates, forget_bias[None], state_m.T, state_n, state_c)

    mixed = pl.pallas_call(
        rest_kernel,
        out_shape=struct((batch, width), bf16),
        in_specs=[VMEM_SPEC] * 3 + [HBM_SPEC] * 4,
        out_specs=VMEM_SPEC,
        scratch_shapes=[pltpu.VMEM(w.shape, bf16) for w in rest_weights]
        + [
            pltpu.VMEM((count, rows, value_width), bf16),
            pltpu.VMEM((tps, batch, width), bf16),
            pltpu.VMEM((tps, batch, width), bf16),
        ]
        + [
            pltpu.VMEM((inner, outer, rows, hidden), bf16),
            pltpu.VMEM((inner, outer, rows, hidden), bf16),
            pltpu.VMEM((outer, rows, hidden), bf16),
            pltpu.VMEM((outer, rows, hidden), bf16),
        ]
        * 2
        + [
            pltpu.VMEM((count, rows, LANES), f32),
            pltpu.VMEM((count, rows, LANES), f32),
            pltpu.VMEM((outer, inner, rows, hidden), bf16),
            sem((4,)),
            sem((count,)),
            sem((count,)),
            sem((tps,)),
            sem((tps,)),
            sem((tps,)),
            sem((tps,)),
            sem((count,)),
            sem((count,)),
            sem((2 * spans, inner)),
            sem((2 * spans, inner)),
            sem((2 * spans, outer)),
            sem((2 * spans, outer)),
            sem((outer,)),
            sem((outer,)),
            sem((outer, inner)),
            sem((outer, inner)),
        ],
        compiler_params=pltpu.CompilerParams(
            collective_id=1, has_side_effects=True, vmem_limit_bytes=VMEM_ALL - SLACK
        ),
        name="rest",
    )(head_out, tokens, mlp_gain[None], *rest_weights)
    return (mixed, new_c, new_n, new_m.T)


def solution(mesh):
    placed = (
        P(None, "kv"),
        P("kv"),
        P("kv", "tp"),
        P("kv", "tp"),
        P("kv", "tp"),
        P("kv", "tp"),
        P(),
        P(),
        P("kv", "tp", None, None),
        P("kv", "tp", None),
        P("kv", "tp"),
        P("tp", "kv"),
        P("kv"),
        P("kv", "tp"),
        P("kv", "tp"),
        P("tp", "kv"),
    )
    return jax.shard_map(
        per_device,
        mesh=mesh,
        in_specs=placed,
        out_specs=(P(None, "kv"), P("kv", "tp", None, None), P("kv", "tp", None), P("kv", "tp")),
        check_vma=False,
    )
```
